32 devices in a mesh: sp: 8 (over z, x), tp: 4 (over y, core).
Axes of the slice: x: 2, y: 2, z: 4, core: 2. Of those that a mesh axis runs over, the one named last changes fastest.
Arguments:
- hidden_in: bfloat16 [512, 2048], P(('sp', 'tp')), may hold values from -6 to 6
- pre_gain: float32 [2048], replicated, may hold values from 0.5 to 1.5
- w_query: bfloat16 [2048, 1024], P(None, 'tp'), may hold values from -0.4375 to 0.4375
- w_key: bfloat16 [2048, 1024], P(None, 'tp'), may hold values from -0.125 to 0.125
- w_value: bfloat16 [2048, 1024], P(None, 'tp'), may hold values from -0.125 to 0.125
- stick_offset: float32 [8], P('tp'), may hold values from -15.2 to -14.2
- w_glu_a: bfloat16 [2048, 1024], P(None, 'tp'), may hold values from -0.125 to 0.125
- w_glu_b: bfloat16 [2048, 1024], P(None, 'tp'), may hold values from -0.125 to 0.125
- w_gate_attn: bfloat16 [2048, 2048], P(None, 'tp'), may hold values from -0.125 to 0.125
- w_gate_conv: bfloat16 [2048, 2048], P(None, 'tp'), may hold values from -0.125 to 0.125
- conv_taps: float32 [31, 1024], P(None, 'tp'), may hold values from -1 to 1
- conv_bias: float32 [1024], P('tp'), may hold values from -0.6 to 0.6
- norm_gain: float32 [1024], P('tp'), may hold values from 0.5 to 1.5
- norm_shift: float32 [1024], P('tp'), may hold values from -0.6 to 0.6
- w_attn_out: bfloat16 [1024, 2048], P('tp'), may hold values from -0.4375 to 0.4375
- w_conv_out: bfloat16 [1024, 2048], P('tp'), may hold values from -0.1875 to 0.1875
- post_gain: float32 [2048], P('tp'), may hold values from 0.5 to 1.5
Outputs:
- mixed: bfloat16 [512, 2048], P('sp', 'tp')
The draws below stay inside these ranges and needn't reach their ends.
All inputs are finite; a program needn't handle non-finite values.
Results may differ from the reference program's by a relative error of at most 0.015.
Values may be sent and summed in bfloat16 or wider, within the bound.
A program may use at most 64 MiB of HBM per device.

```python
import math
import jax
import jax.numpy as jnp
from jax import lax

D = 2048
HEADS = 8
HEAD_DIM = 128
CONV_CH = 1024
WIDTH = 31
TOK_DEV = 64
TOKENS = 512
N_SP = 8


def block_scale(stream_key, dims, shards, least, top_value):
    gain = 1.0
    for position, blocks in shards:
        steps = jax.random.uniform(jax.random.fold_in(jax.random.fold_in(stream_key, 6), position), (blocks,), jnp.float32, least / len(shards), top_value / len(shards))
        gain = gain * jnp.repeat(jnp.exp(steps), dims[position] // blocks).reshape((-1,) + (1,) * (len(dims) - 1 - position))
    return gain


def centred(rng, extent, deviation, limit, shards=(), held_as=jnp.bfloat16):
    result = jax.random.normal(rng, extent, jnp.float32) * deviation
    if len(shards) > 0:
        result = block_scale(rng, extent, shards, -0.22, 0.18) * result
    return jnp.clip(result, min=-limit, max=limit).astype(held_as)


def setup_inputs(seed: int = 0) -> dict:
    key_of = jax.random.split(jax.random.key(seed), 18)
    return {
        "hidden_in": centred(key_of[0], (TOKENS, D), 1.0, 6.0, ((0, 32),)),
        "pre_gain": jnp.clip(1.0 + 0.1 * jax.random.normal(key_of[1], (D,), jnp.float32), 0.5, 1.5),
        "w_query": centred(key_of[2], (D, HEADS * HEAD_DIM), (D // 12) ** -0.5, 0.4375, ((1, 4),)),
        "w_key": centred(key_of[3], (D, HEADS * HEAD_DIM), D ** -0.5, 0.125, ((1, 4),)),
        "w_value": centred(key_of[4], (D, HEADS * HEAD_DIM), D ** -0.5, 0.125, ((1, 4),)),
        "stick_offset": jnp.clip(-15.2 + 1.0 * jax.random.uniform(key_of[5], (HEADS,), jnp.float32) ** block_scale(key_of[5], (HEADS,), ((0, 4),), -0.2, 0.2), -15.2, -14.2),
        "w_glu_a": centred(key_of[6], (D, CONV_CH), D ** -0.5, 0.125, ((1, 4),)),
        "w_glu_b": centred(key_of[7], (D, CONV_CH), D ** -0.5, 0.125, ((1, 4),)),
        "w_gate_attn": centred(key_of[8], (D, D), D ** -0.5, 0.125, ((1, 4),)),
        "w_gate_conv": centred(key_of[9], (D, D), D ** -0.5, 0.125, ((1, 4),)),
        "conv_taps": centred(key_of[10], (WIDTH, CONV_CH), WIDTH ** -0.5, 1.0, ((1, 4),), jnp.float32),
        "conv_bias": centred(key_of[11], (CONV_CH,), 0.1, 0.6, ((0, 4),), jnp.float32),
        "norm_gain": jnp.clip(1.0 + 0.1 * jax.random.normal(key_of[12], (CONV_CH,), jnp.float32), 0.5, 1.5),
        "norm_shift": centred(key_of[13], (CONV_CH,), 0.1, 0.6, ((0, 4),), jnp.float32),
        "w_attn_out": centred(key_of[14], (HEADS * HEAD_DIM, D), (HEADS * HEAD_DIM // 6) ** -0.5, 0.4375, ((0, 4),)),
        "w_conv_out": centred(key_of[15], (CONV_CH, D), CONV_CH ** -0.5, 0.1875, ((0, 4),)),
        "post_gain": jnp.clip(1.0 + 0.1 * jax.random.normal(key_of[16], (D,), jnp.float32), 0.5, 1.5),
    }


epsilon = 1e-06

def held_bf16(values):
    return lax.optimization_barrier(values.astype(jnp.bfloat16))

def reference(hidden_in, pre_gain, w_query, w_key, w_value, stick_offset, w_glu_a, w_glu_b, w_gate_attn, w_gate_conv, conv_taps, conv_bias, norm_gain, norm_shift, w_attn_out, w_conv_out, post_gain):
    values = hidden_in.astype(jnp.float32)
    inverse = lax.rsqrt(lax.optimization_barrier(jnp.mean(values * values, axis=1, keepdims=True)) + epsilon)
    normed = (values * inverse * pre_gain).astype(jnp.bfloat16)

    def project(weight):
        return held_bf16(jnp.dot(normed, weight, preferred_element_type=jnp.float32))
    queries = project(w_query).astype(jnp.float32).reshape(TOKENS, HEADS, HEAD_DIM)
    key_rows = project(w_key).astype(jnp.float32).reshape(TOKENS, HEADS, HEAD_DIM)
    value_rows = project(w_value).astype(jnp.float32).reshape(TOKENS, HEADS, HEAD_DIM)
    glu_left = project(w_glu_a).astype(jnp.float32)
    glu_right = project(w_glu_b).astype(jnp.float32)
    gate_attn = project(w_gate_attn).astype(jnp.float32)
    gate_conv = project(w_gate_conv).astype(jnp.float32)
    positions = jnp.arange(TOKENS, dtype=jnp.int32)

    def attend_block(block_start):
        query_block = lax.dynamic_slice_in_dim(queries, block_start, TOK_DEV, 0)
        scores = jnp.einsum('thd,shd->hts', query_block, key_rows, precision=lax.Precision.HIGHEST)
        scores = scores / math.sqrt(HEAD_DIM) + stick_offset[:, None, None]
        query_pos = block_start + jnp.arange(TOK_DEV, dtype=jnp.int32)
        causal = (positions[None, :] < query_pos[:, None])[None]
        log_rest = jnp.where(causal, jax.nn.log_sigmoid(-scores), 0.0)
        suffix = lax.cumsum(log_rest, axis=2, reverse=True) - log_rest
        weights = jnp.where(causal, jnp.exp(jax.nn.log_sigmoid(scores) + suffix), 0.0)
        return jnp.einsum('hts,shd->thd', weights, value_rows, precision=lax.Precision.HIGHEST)
    starts = jnp.arange(N_SP, dtype=jnp.int32) * TOK_DEV
    attended = lax.map(attend_block, starts).reshape(TOKENS, HEADS * HEAD_DIM).astype(jnp.bfloat16)
    attn_branch = held_bf16(jnp.dot(attended, w_attn_out, preferred_element_type=jnp.float32)).astype(jnp.float32)
    gated_in = held_bf16(glu_left * jax.nn.sigmoid(glu_right)).astype(jnp.float32)
    padded = jnp.pad(gated_in, ((WIDTH - 1, 0), (0, 0)))
    convolved = lax.conv_general_dilated(padded[None], conv_taps.reshape(WIDTH, 1, CONV_CH), (1,), 'VALID', dimension_numbers=('NWC', 'WIO', 'NWC'), feature_group_count=CONV_CH, precision=lax.Precision.HIGHEST)[0] + conv_bias
    mean_row = lax.optimization_barrier(jnp.mean(convolved, axis=1, keepdims=True))
    centered = convolved - mean_row
    spread = lax.optimization_barrier(jnp.mean(centered * centered, axis=1, keepdims=True))
    conv_normed = jax.nn.silu(centered * lax.rsqrt(spread + epsilon) * norm_gain + norm_shift).astype(jnp.bfloat16)
    conv_branch = held_bf16(jnp.dot(conv_normed, w_conv_out, preferred_element_type=jnp.float32)).astype(jnp.float32)
    merged = jax.nn.sigmoid(gate_attn) * attn_branch + jax.nn.sigmoid(gate_conv) * conv_branch
    squares = lax.optimization_barrier(jnp.mean(merged * merged, axis=1, keepdims=True))
    return (merged * lax.rsqrt(squares + epsilon) * post_gain).astype(jnp.bfloat16)
```

```python
from functools import partial
import math

import jax
import jax.numpy as jnp
from jax import lax
from jax.experimental import pallas as pl
from jax.experimental.pallas import tpu as pltpu
from jax.sharding import PartitionSpec as P

HEAD_DIM = 128
WIDTH = 31
EPSILON = 1e-06
HALO = 32
MESH = pl.DeviceIdType.MESH


def mm(left, right):
    return jnp.dot(left, right, preferred_element_type=jnp.float32)


def row(ref):
    return ref[...].reshape(1, ref.shape[0])


def whole_layer(
    sp_count,
    tp_count,
    pair,
    hidden_in,
    pre_gain,
    w_query,
    w_key,
    w_value,
    stick_offset,
    w_glu_a,
    w_glu_b,
    w_gate_attn,
    w_gate_conv,
    conv_taps,
    conv_bias,
    norm_gain,
    norm_shift,
    w_attn_out,
    w_conv_out,
    post_gain,
    out,
    hidden_all,
    pre_gain_v,
    wq,
    wk,
    wv,
    wa,
    wb,
    wga,
    wgc,
    taps,
    bias,
    gain,
    shift,
    wo,
    wc,
    post_gain_v,
    normed,
    kv,
    gated,
    gated_f32,
    attn_out,
    attn_in,
    conv_out,
    conv_in,
    stat_out,
    stat_in,
    square_out,
    square_in,
    local_sem,
    hidden_send,
    hidden_recv,
    column_send,
    across_send,
    relay_send,
    kv_recv,
    halo_send,
    halo_recv,
    attn_send,
    attn_recv,
    conv_send,
    conv_recv,
    stat_send,
    stat_recv,
    square_send,
    square_recv,
):
    part, width = hidden_in.shape
    rows = part * tp_count
    channels = w_glu_a.shape[1]
    kv_width = w_key.shape[1]
    heads = stick_offset.shape[0]
    out_cols = post_gain.shape[0]
    outer = sp_count // pair
    sp = lax.axis_index("sp")
    tp = lax.axis_index("tp")
    z, x = sp // pair, sp % pair
    f32, bf16 = jnp.float32, jnp.bfloat16

    local_pairs = (
        (hidden_in, hidden_all.at[tp]),
        (pre_gain, pre_gain_v),
        (w_key, wk),
        (w_value, wv),
        (w_glu_a, wa),
        (w_glu_b, wb),
        (w_query, wq),
        (conv_taps, taps),
        (conv_bias, bias),
        (norm_gain, gain),
        (norm_shift, shift),
        (w_gate_attn, wga),
        (w_gate_conv, wgc),
        (w_conv_out, wc),
        (w_attn_out, wo),
        (post_gain, post_gain_v),
    )
    loads = [
        pltpu.make_async_copy(source, target, local_sem.at[index])
        for index, (source, target) in enumerate(local_pairs)
    ]
    (
        l_hidden, l_pre, l_key, l_value, l_a, l_b, l_query, l_taps, l_bias, l_gain, l_shift,
        l_ga, l_gc, l_wc, l_wo, l_post,
    ) = loads
    for load in loads:
        load.start()

    barrier = pltpu.get_barrier_semaphore()

    def greet(sp_index, tp_index):
        pl.semaphore_signal(barrier, inc=1, device_id=(sp_index, tp_index), device_id_type=MESH)

    for step in range(1, tp_count):
        greet(sp, lax.rem(tp + step, tp_count))
    for step in range(1, outer):
        greet(lax.rem(z + step, outer) * pair + x, tp)
    if pair == 2:
        greet(z * pair + (1 - x), tp)
    greetings = tp_count - 1 + outer - 1 + (pair - 1)
    if pair == 2:
        with_next = (x == 1) & (z < outer - 1)
        with_previous = (x == 0) & (z > 0)

        @pl.when(with_next)
        def _():
            greet(sp + 1, tp)

        @pl.when(with_previous)
        def _():
            greet(sp - 1, tp)

        greetings = greetings + jnp.where(with_next | with_previous, 1, 0)

    pl.semaphore_wait(barrier, greetings)

    def remote(source, target, send_sem, recv_sem, sp_index, tp_index):
        return pltpu.make_async_remote_copy(
            src_ref=source,
            dst_ref=target,
            send_sem=send_sem,
            recv_sem=recv_sem,
            device_id=(sp_index, tp_index),
            device_id_type=MESH,
        )

    peers = [lax.rem(tp + step, tp_count) for step in range(1, tp_count)]

    def exchange(source, target, send_sem, recv_sem, peer, varied):
        piece = source.at[peer] if varied else source
        return remote(piece, target.at[tp], send_sem.at[peer], recv_sem.at[tp], sp, peer)

    def arrival(target, send_sem, recv_sem, peer):
        return remote(
            target.at[peer], target.at[peer], send_sem.at[peer], recv_sem.at[peer], sp, peer
        )

    l_hidden.wait()
    hidden_copies = [
        exchange(hidden_all.at[tp], hidden_all, hidden_send, hidden_recv, peer, False)
        for peer in peers
    ]
    for copy in hidden_copies:
        copy.start()
    l_pre.wait()
    for peer in peers:
        arrival(hidden_all, hidden_send, hidden_recv, peer).wait_recv()
    for index in range(tp_count):
        values = hidden_all[index].astype(f32)
        inverse = lax.rsqrt(jnp.mean(values * values, axis=1, keepdims=True) + EPSILON)
        normed[index * part : (index + 1) * part, :] = (
            values * inverse * row(pre_gain_v)
        ).astype(bf16)

    def project(weight):
        return mm(normed[...], weight[...]).astype(bf16)

    l_key.wait()
    kv[sp, :, :kv_width] = project(wk)
    l_value.wait()
    kv[sp, :, kv_width:] = project(wv)

    def column_copy(target_z):
        return remote(
            kv.at[sp], kv.at[sp], column_send.at[target_z], kv_recv.at[sp],
            target_z * pair + x, tp,
        )

    def across_copy():
        return remote(kv.at[sp], kv.at[sp], across_send, kv_recv.at[sp], sp + 1, tp)

    def relay_copy(source_z):
        block = source_z * pair + x
        return remote(
            kv.at[block], kv.at[block], relay_send.at[source_z], kv_recv.at[block],
            z * pair + (1 - x), tp,
        )

    def block_arrival(block):
        return remote(
            kv.at[block], kv.at[block], across_send, kv_recv.at[block], sp, lax.rem(tp + 1, tp_count)
        )

    if pair == 2:

        @pl.when(x == 0)
        def _():
            across_copy().start()
            kv[sp + 1] = jnp.zeros(kv.shape[1:], bf16)

    @pl.loop(z + 1, outer)
    def _(target_z):
        column_copy(target_z).start()

    def relay(source_z):
        block_arrival(source_z * pair + x).wait_recv()
        if pair == 2:
            relay_copy(source_z).start()

    l_a.wait()
    left = project(wa).astype(f32)
    l_b.wait()
    right = project(wb).astype(f32)
    gated[HALO:, :] = (left * jax.nn.sigmoid(right)).astype(bf16)

    def halo_copy():
        return remote(
            gated.at[pl.ds(rows, HALO)], gated.at[pl.ds(0, HALO)], halo_send, halo_recv,
            jnp.minimum(sp + 1, sp_count - 1) if pair == 1 else sp + 1, tp,
        )

    @pl.when(sp < sp_count - 1)
    def _():
        halo_copy().start()

    @pl.when(sp == 0)
    def _():
        gated[:HALO, :] = jnp.zeros((HALO, channels), bf16)

    l_query.wait()
    queries = project(wq)

    early = min(outer - 1, 3)

    def early_relay(step):
        if step <= early:

            @pl.when(z >= step)
            def _():
                relay(z - step)

    early_relay(1)
    l_ga.wait()
    gate_attn = jax.nn.sigmoid(project(wga).astype(f32))
    early_relay(2)
    l_gc.wait()
    gate_conv = jax.nn.sigmoid(project(wgc).astype(f32))
    early_relay(3)

    @pl.when(sp > 0)
    def _():
        halo_copy().wait_recv()

    for load in (l_taps, l_bias, l_gain, l_shift):
        load.wait()
    gated_f32[...] = gated[...].astype(f32)
    sums = [jnp.broadcast_to(row(bias), (rows, channels))] + [jnp.zeros((rows, channels), f32)] * 3
    for tap in range(WIDTH):
        first = HALO - (WIDTH - 1) + tap
        sums[tap % 4] = sums[tap % 4] + taps[tap : tap + 1, :] * gated_f32[first : first + rows, :]
    convolved = (sums[0] + sums[1]) + (sums[2] + sums[3])

    def turned(columns):
        lane = lax.broadcasted_iota(jnp.int32, (rows, 128), 1)
        tile = jnp.zeros((rows, 128), f32)
        for index, column in enumerate(columns):
            tile = jnp.where(lane == index, column, tile)
        return jnp.transpose(tile)[:8, :]

    def turned_back(tile):
        full = jnp.concatenate([tile, jnp.zeros((120, rows), f32)], axis=0)
        return jnp.transpose(full)

    stat_out[...] = turned(
        [
            jnp.sum(convolved, axis=1, keepdims=True),
            jnp.sum(convolved * convolved, axis=1, keepdims=True),
        ]
    )
    for peer in peers:
        exchange(stat_out, stat_in, stat_send, stat_recv, peer, False).start()

    stacked = heads * rows
    scale = 1.0 / math.sqrt(HEAD_DIM)
    keys_step = pair * rows
    offset_column = jnp.concatenate(
        [jnp.full((rows, 1), stick_offset[head], f32) for head in range(heads)], axis=0
    )
    later = (
        lax.broadcasted_iota(jnp.int32, (keys_step, keys_step), 0)
        > lax.broadcasted_iota(jnp.int32, (keys_step, keys_step), 1)
    ).astype(bf16)

    def attend(pair_index, state, causal):
        total, summed = state
        blocks = kv[pl.ds(pair_index * pair, pair)].reshape(keys_step, 2 * kv_width)
        scores = jnp.concatenate(
            [
                lax.dot_general(
                    queries[:, head * HEAD_DIM : (head + 1) * HEAD_DIM],
                    blocks[:, head * HEAD_DIM : (head + 1) * HEAD_DIM],
                    (((1,), (1,)), ((), ())),
                    preferred_element_type=f32,
                )
                for head in range(heads)
            ],
            axis=0,
        )
        scores = scores * scale + offset_column
        small = jnp.log(1.0 + jnp.exp(-jnp.abs(scores)))
        rest = -(jnp.maximum(scores, 0.0) + small)
        if causal is not None:
            rest = jnp.where(causal, rest, 0.0)
        high = rest.astype(bf16)
        low = (rest - high.astype(f32)).astype(bf16)
        inside = mm(high, later) + mm(low, later)
        weights = jnp.exp(jnp.minimum(scores, 0.0) - small + inside + total)
        if causal is not None:
            weights = jnp.where(causal, weights, 0.0)
        weights = weights.astype(bf16)
        added = jnp.concatenate(
            [
                mm(
                    weights[head * rows : (head + 1) * rows],
                    blocks[:, kv_width + head * HEAD_DIM : kv_width + (head + 1) * HEAD_DIM],
                )
                for head in range(heads)
            ],
            axis=0,
        )
        return (total + jnp.sum(rest, axis=1, keepdims=True), summed + added)

    if pair == 2:

        @pl.when(x == 1)
        def _():
            block_arrival(sp - 1).wait_recv()

    token = lax.broadcasted_iota(jnp.int32, (rows, keys_step), 0)
    token = jnp.concatenate([token] * heads, axis=0) + x * rows
    causal = lax.broadcasted_iota(jnp.int32, (stacked, keys_step), 1) < token
    state = attend(
        z, (jnp.zeros((stacked, 1), f32), jnp.zeros((stacked, HEAD_DIM), f32)), causal
    )

    stats = stat_out[...]
    for peer in peers:
        arrival(stat_in, stat_send, stat_recv, peer).wait_recv()
        stats = stats + stat_in[peer]
    stats = turned_back(stats) / (channels * tp_count)
    mean = stats[:, 0:1]
    spread = stats[:, 1:2] - mean * mean
    conv_normed = jax.nn.silu(
        (convolved - mean) * lax.rsqrt(spread + EPSILON) * row(gain) + row(shift)
    ).astype(bf16)

    def branch(values, weight, sent, received, send_sem, recv_sem):
        def term(peer):
            return mm(values, weight[:, pl.ds(pl.multiple_of(peer * out_cols, 128), out_cols)])

        for peer in peers:
            sent[peer] = term(peer).astype(bf16)
            exchange(sent, received, send_sem, recv_sem, peer, True).start()
        return term(tp)

    def branch_sum(own, received, send_sem, recv_sem):
        for peer in peers:
            arrival(received, send_sem, recv_sem, peer).wait_recv()
            own = own + received[peer].astype(f32)
        return own.astype(bf16).astype(f32)

    l_wc.wait()
    conv_own = branch(conv_normed, wc, conv_out, conv_in, conv_send, conv_recv)

    def earlier(step, state):
        source_z = z - step
        if outer - 1 > early:

            @pl.when(step > early)
            def _():
                relay(source_z)

        if pair == 2:
            block_arrival(source_z * pair + (1 - x)).wait_recv()
        return attend(source_z, state, None)

    _, summed = lax.fori_loop(1, z + 1, earlier, state)
    attended = jnp.concatenate(
        [summed[head * rows : (head + 1) * rows] for head in range(heads)], axis=1
    ).astype(bf16)

    l_wo.wait()
    attn_own = branch(attended, wo, attn_out, attn_in, attn_send, attn_recv)
    merged = gate_conv * branch_sum(conv_own, conv_in, conv_send, conv_recv)
    merged = gate_attn * branch_sum(attn_own, attn_in, attn_send, attn_recv) + merged

    square_out[...] = turned([jnp.sum(merged * merged, axis=1, keepdims=True)])
    for peer in peers:
        exchange(square_out, square_in, square_send, square_recv, peer, False).start()
    l_post.wait()
    scaled = merged * row(post_gain_v)
    squares = square_out[...]
    for peer in peers:
        arrival(square_in, square_send, square_recv, peer).wait_recv()
        squares = squares + square_in[peer]
    squares = turned_back(squares)[:, 0:1]
    out[...] = (scaled * lax.rsqrt(squares / width + EPSILON)).astype(bf16)

    for peer in peers:
        exchange(hidden_all.at[tp], hidden_all, hidden_send, hidden_recv, peer, False).wait_send()
        exchange(stat_out, stat_in, stat_send, stat_recv, peer, False).wait_send()
        exchange(conv_out, conv_in, conv_send, conv_recv, peer, True).wait_send()
        exchange(attn_out, attn_in, attn_send, attn_recv, peer, True).wait_send()
        exchange(square_out, square_in, square_send, square_recv, peer, False).wait_send()
    if pair == 2:

        @pl.when(x == 0)
        def _():
            across_copy().wait_send()

    @pl.loop(z + 1, outer)
    def _(target_z):
        column_copy(target_z).wait_send()

    if pair == 2:

        @pl.loop(0, z)
        def _(source_z):
            relay_copy(source_z).wait_send()

    @pl.when(sp < sp_count - 1)
    def _():
        halo_copy().wait_send()


def shards(sp_count, tp_count, *arguments):
    (
        hidden_in, pre_gain, w_query, w_key, w_value, stick_offset, w_glu_a, w_glu_b,
        w_gate_attn, w_gate_conv, conv_taps, conv_bias, norm_gain, norm_shift,
        w_attn_out, w_conv_out, post_gain,
    ) = arguments
    pair = 2 if sp_count % 2 == 0 else 1
    part, width = hidden_in.shape
    rows = part * tp_count
    channels = w_glu_a.shape[1]
    kv_width = w_key.shape[1]
    out_cols = post_gain.shape[0]
    outer = sp_count // pair
    f32, bf16 = jnp.float32, jnp.bfloat16
    dma = pltpu.SemaphoreType.DMA

    def like(array):
        return pltpu.VMEM(array.shape, array.dtype)

    in_specs = [
        pl.BlockSpec(memory_space=pltpu.SMEM if index == 5 else pl.ANY)
        for index in range(len(arguments))
    ]
    branch_shape = (tp_count, rows, out_cols)
    return pl.pallas_call(
        partial(whole_layer, sp_count, tp_count, pair),
        out_shape=jax.ShapeDtypeStruct((rows, out_cols), bf16),
        in_specs=in_specs,
        out_specs=pl.BlockSpec(memory_space=pltpu.VMEM),
        scratch_shapes=[
            pltpu.VMEM((tp_count, part, width), bf16),
            like(pre_gain),
            like(w_query),
            like(w_key),
            like(w_value),
            like(w_glu_a),
            like(w_glu_b),
            like(w_gate_attn),
            like(w_gate_conv),
            like(conv_taps),
            like(conv_bias),
            like(norm_gain),
            like(norm_shift),
            like(w_attn_out),
            like(w_conv_out),
            like(post_gain),
            pltpu.VMEM((rows, width), bf16),
            pltpu.VMEM((sp_count, rows, 2 * kv_width), bf16),
            pltpu.VMEM((HALO + rows, channels), bf16),
            pltpu.VMEM((HALO + rows, channels), f32),
            pltpu.VMEM(branch_shape, bf16),
            pltpu.VMEM(branch_shape, bf16),
            pltpu.VMEM(branch_shape, bf16),
            pltpu.VMEM(branch_shape, bf16),
            pltpu.VMEM((8, rows), f32),
            pltpu.VMEM((tp_count, 8, rows), f32),
            pltpu.VMEM((8, rows), f32),
            pltpu.VMEM((tp_count, 8, rows), f32),
            dma((16,)),
            dma((tp_count,)),
            dma((tp_count,)),
            dma((outer,)),
            dma,
            dma((outer,)),
            dma((sp_count,)),
            dma,
            dma,
            dma((tp_count,)),
            dma((tp_count,)),
            dma((tp_count,)),
            dma((tp_count,)),
            dma((tp_count,)),
            dma((tp_count,)),
            dma((tp_count,)),
            dma((tp_count,)),
        ],
        compiler_params=pltpu.CompilerParams(
            collective_id=0, has_side_effects=True, vmem_limit_bytes=60 * 1024 * 1024
        ),
    )(*arguments)


def solution(mesh):
    in_specs = (
        P(("sp", "tp"), None),
        P(),
        P(None, "tp"),
        P(None, "tp"),
        P(None, "tp"),
        P("tp"),
        P(None, "tp"),
        P(None, "tp"),
        P(None, "tp"),
        P(None, "tp"),
        P(None, "tp"),
        P("tp"),
        P("tp"),
        P("tp"),
        P("tp", None),
        P("tp", None),
        P("tp"),
    )
    body = partial(shards, mesh.shape["sp"], mesh.shape["tp"])
    return jax.shard_map(
        body, mesh=mesh, in_specs=in_specs, out_specs=P("sp", "tp"), check_vma=False
    )
```

```python
from functools import partial
import math

import jax
import jax.numpy as jnp
from jax import lax
from jax.experimental import pallas as pl
from jax.experimental.pallas import tpu as pltpu
from jax.sharding import PartitionSpec as P

HEAD_DIM = 128
WIDTH = 31
EPSILON = 1e-06
HALO = 32
MESH = pl.DeviceIdType.MESH


def mm(left, right):
    return jnp.dot(left, right, preferred_element_type=jnp.float32)


def row(ref):
    return ref[...].reshape(1, ref.shape[0])


def whole_layer(
    sp_count,
    tp_count,
    pair,
    hidden_in,
    pre_gain,
    w_query,
    w_key,
    w_value,
    stick_offset,
    w_glu_a,
    w_glu_b,
    w_gate_attn,
    w_gate_conv,
    conv_taps,
    conv_bias,
    norm_gain,
    norm_shift,
    w_attn_out,
    w_conv_out,
    post_gain,
    out,
    hidden_all,
    pre_gain_v,
    wq,
    wk,
    wv,
    wa,
    wb,
    wga,
    wgc,
    taps,
    bias,
    gain,
    shift,
    wo,
    wc,
    post_gain_v,
    normed,
    kv,
    gated,
    gated_f32,
    attn_out,
    attn_in,
    conv_out,
    conv_in,
    stat_out,
    stat_in,
    square_out,
    square_in,
    local_sem,
    ready,
    hidden_send,
    hidden_recv,
    column_send,
    across_send,
    relay_send,
    kv_recv,
    halo_send,
    halo_recv,
    attn_send,
    attn_recv,
    conv_send,
    conv_recv,
    stat_send,
    stat_recv,
    square_send,
    square_recv,
):
    part, width = hidden_in.shape
    rows = part * tp_count
    channels = w_glu_a.shape[1]
    kv_width = w_key.shape[1]
    heads = stick_offset.shape[0]
    out_cols = post_gain.shape[0]
    outer = sp_count // pair
    size = 2 if tp_count % 2 == 0 else 1
    groups = tp_count // size
    sp = lax.axis_index("sp")
    tp = lax.axis_index("tp")
    z, x = sp // pair, sp % pair
    f32, bf16 = jnp.float32, jnp.bfloat16

    local_pairs = (
        (hidden_in, hidden_all.at[tp]),
        (pre_gain, pre_gain_v),
        (w_key, wk),
        (w_value, wv),
        (w_glu_a, wa),
        (w_glu_b, wb),
        (w_query, wq),
        (conv_taps, taps),
        (conv_bias, bias),
        (norm_gain, gain),
        (norm_shift, shift),
        (w_gate_attn, wga),
        (w_gate_conv, wgc),
        (w_conv_out, wc),
        (w_attn_out, wo),
        (post_gain, post_gain_v),
    )
    loads = [
        pltpu.make_async_copy(source, target, local_sem.at[index])
        for index, (source, target) in enumerate(local_pairs)
    ]
    (
        l_hidden, l_pre, l_key, l_value, l_a, l_b, l_query, l_taps, l_bias, l_gain, l_shift,
        l_ga, l_gc, l_wc, l_wo, l_post,
    ) = loads
    for load in loads:
        load.start()

    barrier = pltpu.get_barrier_semaphore()

    def greet(sp_index, tp_index):
        pl.semaphore_signal(barrier, inc=1, device_id=(sp_index, tp_index), device_id_type=MESH)

    for step in range(1, tp_count):
        greet(sp, lax.rem(tp + step, tp_count))
    if pair == 2:
        greet(z * pair + (1 - x), tp)

    @pl.when(z > 0)
    def _():
        greet(sp - pair, tp)

    @pl.when(z < outer - 1)
    def _():
        greet(sp + pair, tp)

    beside = jnp.where(z > 0, 1, 0) + jnp.where(z < outer - 1, 1, 0)
    pl.semaphore_wait(barrier, tp_count - 1 + (pair - 1) + beside)

    def remote(source, target, send_sem, recv_sem, sp_index, tp_index):
        return pltpu.make_async_remote_copy(
            src_ref=source,
            dst_ref=target,
            send_sem=send_sem,
            recv_sem=recv_sem,
            device_id=(sp_index, tp_index),
            device_id_type=MESH,
        )

    peers = [lax.rem(tp + step, tp_count) for step in range(1, tp_count)]

    def exchange(source, target, send_sem, recv_sem, peer, varied):
        piece = source.at[peer] if varied else source
        return remote(piece, target.at[tp], send_sem.at[peer], recv_sem.at[tp], sp, peer)

    def arrival(target, send_sem, recv_sem, peer):
        return remote(
            target.at[peer], target.at[peer], send_sem.at[peer], recv_sem.at[peer], sp, peer
        )

    l_hidden.wait()
    hidden_copies = [
        exchange(hidden_all.at[tp], hidden_all, hidden_send, hidden_recv, peer, False)
        for peer in peers
    ]
    for copy in hidden_copies:
        copy.start()

    @pl.when(z < outer - 1)
    def _():
        pl.semaphore_wait(ready, 1)

    @pl.when(z > 0)
    def _():
        pl.semaphore_signal(ready, inc=1, device_id=(sp - pair, tp), device_id_type=MESH)

    l_pre.wait()

    def project(weight):
        return mm(normed[...], weight[...]).astype(bf16)

    def group_rows(group):
        first = lax.rem(tp // size + group, groups) * (size * part)
        return pl.ds(pl.multiple_of(first, size * part), size * part)

    def kv_copy(block, group, send_sem, sp_index):
        piece = kv.at[block, group_rows(group)]
        return remote(piece, piece, send_sem, kv_recv.at[block, group], sp_index, tp)

    def column_copy(target_z, group):
        return kv_copy(sp, group, column_send.at[target_z, group], target_z * pair + x)

    def across_copy(group):
        return kv_copy(sp, group, across_send.at[group], sp + 1)

    def relay_copy(source_z, group):
        return kv_copy(
            source_z * pair + x, group, relay_send.at[source_z, group], z * pair + (1 - x)
        )

    def block_arrival(block, group):
        piece = kv.at[block, group_rows(group)]
        return remote(
            piece, piece, across_send.at[group], kv_recv.at[block, group], sp,
            lax.rem(tp + 1, tp_count),
        )

    def relay(source_z, group):
        block_arrival(source_z * pair + x, group).wait_recv()
        if pair == 2:
            relay_copy(source_z, group).start()

    for group in range(groups):
        for member in range(size):
            index = lax.rem(tp // size + group, groups) * size + member
            if group == 0:

                @pl.when(index != tp)
                def _():
                    arrival(hidden_all, hidden_send, hidden_recv, index).wait_recv()

            else:
                arrival(hidden_all, hidden_send, hidden_recv, index).wait_recv()
            values = hidden_all[index].astype(f32)
            inverse = lax.rsqrt(jnp.mean(values * values, axis=1, keepdims=True) + EPSILON)
            normed[pl.ds(pl.multiple_of(index * part, part), part), :] = (
                values * inverse * row(pre_gain_v)
            ).astype(bf16)
        if group == 0:
            l_key.wait()
            l_value.wait()
        tokens = normed[group_rows(group), :]
        kv[sp, group_rows(group), :kv_width] = mm(tokens, wk[...]).astype(bf16)
        kv[sp, group_rows(group), kv_width:] = mm(tokens, wv[...]).astype(bf16)
        if pair == 2:

            @pl.when(x == 0)
            def _():
                across_copy(group).start()

        @pl.loop(z + 1, outer)
        def _(target_z):
            column_copy(target_z, group).start()

    if pair == 2:

        @pl.when(x == 0)
        def _():
            kv[sp + 1] = jnp.zeros(kv.shape[1:], bf16)

    def early_relay(group, step):
        if step <= early and group < groups:

            @pl.when(z >= step)
            def _():
                relay(z - step, group)

    early = min(outer - 1, 3)

    l_a.wait()
    left = project(wa).astype(f32)
    l_b.wait()
    right = project(wb).astype(f32)
    gated[HALO:, :] = (left * jax.nn.sigmoid(right)).astype(bf16)

    def halo_copy():
        return remote(
            gated.at[pl.ds(rows, HALO)], gated.at[pl.ds(0, HALO)], halo_send, halo_recv,
            jnp.minimum(sp + 1, sp_count - 1) if pair == 1 else sp + 1, tp,
        )

    @pl.when(sp < sp_count - 1)
    def _():
        halo_copy().start()

    @pl.when(sp == 0)
    def _():
        gated[:HALO, :] = jnp.zeros((HALO, channels), bf16)

    early_relay(0, 1)
    l_query.wait()
    queries = project(wq)

    early_relay(0, 2)
    l_ga.wait()
    gate_attn = jax.nn.sigmoid(project(wga).astype(f32))
    early_relay(0, 3)
    l_gc.wait()
    gate_conv = jax.nn.sigmoid(project(wgc).astype(f32))
    early_relay(1, 1)

    @pl.when(sp > 0)
    def _():
        halo_copy().wait_recv()

    for load in (l_taps, l_bias, l_gain, l_shift):
        load.wait()
    gated_f32[...] = gated[...].astype(f32)
    sums = [jnp.broadcast_to(row(bias), (rows, channels))] + [jnp.zeros((rows, channels), f32)] * 3
    for tap in range(WIDTH):
        first = HALO - (WIDTH - 1) + tap
        sums[tap % 4] = sums[tap % 4] + taps[tap : tap + 1, :] * gated_f32[first : first + rows, :]
    convolved = (sums[0] + sums[1]) + (sums[2] + sums[3])

    def turned(columns):
        lane = lax.broadcasted_iota(jnp.int32, (rows, 128), 1)
        tile = jnp.zeros((rows, 128), f32)
        for index, column in enumerate(columns):
            tile = jnp.where(lane == index, column, tile)
        return jnp.transpose(tile)[:8, :]

    def turned_back(tile):
        full = jnp.concatenate([tile, jnp.zeros((120, rows), f32)], axis=0)
        return jnp.transpose(full)

    stat_out[...] = turned(
        [
            jnp.sum(convolved, axis=1, keepdims=True),
            jnp.sum(convolved * convolved, axis=1, keepdims=True),
        ]
    )
    for peer in peers:
        exchange(stat_out, stat_in, stat_send, stat_recv, peer, False).start()

    stacked = heads * rows
    scale = 1.0 / math.sqrt(HEAD_DIM)
    keys_step = pair * rows
    offset_column = jnp.concatenate(
        [jnp.full((rows, 1), stick_offset[head], f32) for head in range(heads)], axis=0
    )
    later = (
        lax.broadcasted_iota(jnp.int32, (keys_step, keys_step), 0)
        > lax.broadcasted_iota(jnp.int32, (keys_step, keys_step), 1)
    ).astype(bf16)

    def attend(pair_index, state, causal):
        total, summed = state
        blocks = kv[pl.ds(pair_index * pair, pair)].reshape(keys_step, 2 * kv_width)
        scores = jnp.concatenate(
            [
                lax.dot_general(
                    queries[:, head * HEAD_DIM : (head + 1) * HEAD_DIM],
                    blocks[:, head * HEAD_DIM : (head + 1) * HEAD_DIM],
                    (((1,), (1,)), ((), ())),
                    preferred_element_type=f32,
                )
                for head in range(heads)
            ],
            axis=0,
        )
        scores = scores * scale + offset_column
        small = jnp.log(1.0 + jnp.exp(-jnp.abs(scores)))
        rest = -(jnp.maximum(scores, 0.0) + small)
        if causal is not None:
            rest = jnp.where(causal, rest, 0.0)
        high = rest.astype(bf16)
        low = (rest - high.astype(f32)).astype(bf16)
        inside = mm(high, later) + mm(low, later)
        weights = jnp.exp(jnp.minimum(scores, 0.0) - small + inside + total)
        if causal is not None:
            weights = jnp.where(causal, weights, 0.0)
        weights = weights.astype(bf16)
        added = jnp.concatenate(
            [
                mm(
                    weights[head * rows : (head + 1) * rows],
                    blocks[:, kv_width + head * HEAD_DIM : kv_width + (head + 1) * HEAD_DIM],
                )
                for head in range(heads)
            ],
            axis=0,
        )
        return (total + jnp.sum(rest, axis=1, keepdims=True), summed + added)

    if pair == 2:

        @pl.when(x == 1)
        def _():
            for group in range(groups):
                block_arrival(sp - 1, group).wait_recv()

    token = lax.broadcasted_iota(jnp.int32, (rows, keys_step), 0)
    token = jnp.concatenate([token] * heads, axis=0) + x * rows
    causal = lax.broadcasted_iota(jnp.int32, (stacked, keys_step), 1) < token
    state = attend(
        z, (jnp.zeros((stacked, 1), f32), jnp.zeros((stacked, HEAD_DIM), f32)), causal
    )

    stats = stat_out[...]
    for peer in peers:
        arrival(stat_in, stat_send, stat_recv, peer).wait_recv()
        stats = stats + stat_in[peer]
    stats = turned_back(stats) / (channels * tp_count)
    mean = stats[:, 0:1]
    spread = stats[:, 1:2] - mean * mean
    conv_normed = jax.nn.silu(
        (convolved - mean) * lax.rsqrt(spread + EPSILON) * row(gain) + row(shift)
    ).astype(bf16)

    def branch(values, weight, sent, received, send_sem, recv_sem):
        def term(peer):
            return mm(values, weight[:, pl.ds(pl.multiple_of(peer * out_cols, 128), out_cols)])

        for peer in peers:
            sent[peer] = term(peer).astype(bf16)
            exchange(sent, received, send_sem, recv_sem, peer, True).start()
        return term(tp)

    def branch_sum(own, received, send_sem, recv_sem):
        for peer in peers:
            arrival(received, send_sem, recv_sem, peer).wait_recv()
            own = own + received[peer].astype(f32)
        return own.astype(bf16).astype(f32)

    l_wc.wait()
    conv_own = branch(conv_normed, wc, conv_out, conv_in, conv_send, conv_recv)

    @pl.loop(early + 1, z + 1)
    def _(step):
        relay(z - step, 0)

    def earlier(step, state):
        source_z = z - step
        for group in range(1, groups):
            if group > 1:
                relay(source_z, group)
            else:

                @pl.when(step < z)
                def _():
                    relay(source_z - 1, group)

        if pair == 2:
            for group in range(groups):
                block_arrival(source_z * pair + (1 - x), group).wait_recv()
        return attend(source_z, state, None)

    _, summed = lax.fori_loop(1, z + 1, earlier, state)
    attended = jnp.concatenate(
        [summed[head * rows : (head + 1) * rows] for head in range(heads)], axis=1
    ).astype(bf16)

    l_wo.wait()
    attn_own = branch(attended, wo, attn_out, attn_in, attn_send, attn_recv)
    merged = gate_conv * branch_sum(conv_own, conv_in, conv_send, conv_recv)
    merged = gate_attn * branch_sum(attn_own, attn_in, attn_send, attn_recv) + merged

    square_out[...] = turned([jnp.sum(merged * merged, axis=1, keepdims=True)])
    for peer in peers:
        exchange(square_out, square_in, square_send, square_recv, peer, False).start()
    l_post.wait()
    scaled = merged * row(post_gain_v)
    squares = square_out[...]
    for peer in peers:
        arrival(square_in, square_send, square_recv, peer).wait_recv()
        squares = squares + square_in[peer]
    squares = turned_back(squares)[:, 0:1]
    out[...] = (scaled * lax.rsqrt(squares / width + EPSILON)).astype(bf16)

    for peer in peers:
        exchange(hidden_all.at[tp], hidden_all, hidden_send, hidden_recv, peer, False).wait_send()
        exchange(stat_out, stat_in, stat_send, stat_recv, peer, False).wait_send()
        exchange(conv_out, conv_in, conv_send, conv_recv, peer, True).wait_send()
        exchange(attn_out, attn_in, attn_send, attn_recv, peer, True).wait_send()
        exchange(square_out, square_in, square_send, square_recv, peer, False).wait_send()
    for group in range(groups):
        if pair == 2:

            @pl.when(x == 0)
            def _():
                across_copy(group).wait_send()

            @pl.loop(0, z)
            def _(source_z):
                relay_copy(source_z, group).wait_send()

        @pl.loop(z + 1, outer)
        def _(target_z):
            column_copy(target_z, group).wait_send()

    @pl.when(sp < sp_count - 1)
    def _():
        halo_copy().wait_send()


def shards(sp_count, tp_count, *arguments):
    (
        hidden_in, pre_gain, w_query, w_key, w_value, stick_offset, w_glu_a, w_glu_b,
        w_gate_attn, w_gate_conv, conv_taps, conv_bias, norm_gain, norm_shift,
        w_attn_out, w_conv_out, post_gain,
    ) = arguments
    pair = 2 if sp_count % 2 == 0 else 1
    part, width = hidden_in.shape
    rows = part * tp_count
    channels = w_glu_a.shape[1]
    kv_width = w_key.shape[1]
    out_cols = post_gain.shape[0]
    outer = sp_count // pair
    groups = tp_count // (2 if tp_count % 2 == 0 else 1)
    f32, bf16 = jnp.float32, jnp.bfloat16
    dma = pltpu.SemaphoreType.DMA

    def like(array):
        return pltpu.VMEM(array.shape, array.dtype)

    in_specs = [
        pl.BlockSpec(memory_space=pltpu.SMEM if index == 5 else pl.ANY)
        for index in range(len(arguments))
    ]
    branch_shape = (tp_count, rows, out_cols)
    return pl.pallas_call(
        partial(whole_layer, sp_count, tp_count, pair),
        out_shape=jax.ShapeDtypeStruct((rows, out_cols), bf16),
        in_specs=in_specs,
        out_specs=pl.BlockSpec(memory_space=pltpu.VMEM),
        scratch_shapes=[
            pltpu.VMEM((tp_count, part, width), bf16),
            like(pre_gain),
            like(w_query),
            like(w_key),
            like(w_value),
            like(w_glu_a),
            like(w_glu_b),
            like(w_gate_attn),
            like(w_gate_conv),
            like(conv_taps),
            like(conv_bias),
            like(norm_gain),
            like(norm_shift),
            like(w_attn_out),
            like(w_conv_out),
            like(post_gain),
            pltpu.VMEM((rows, width), bf16),
            pltpu.VMEM((sp_count, rows, 2 * kv_width), bf16),
            pltpu.VMEM((HALO + rows, channels), bf16),
            pltpu.VMEM((HALO + rows, channels), f32),
            pltpu.VMEM(branch_shape, bf16),
            pltpu.VMEM(branch_shape, bf16),
            pltpu.VMEM(branch_shape, bf16),
            pltpu.VMEM(branch_shape, bf16),
            pltpu.VMEM((8, rows), f32),
            pltpu.VMEM((tp_count, 8, rows), f32),
            pltpu.VMEM((8, rows), f32),
            pltpu.VMEM((tp_count, 8, rows), f32),
            dma((16,)),
            pltpu.SemaphoreType.REGULAR,
            dma((tp_count,)),
            dma((tp_count,)),
            dma((outer, groups)),
            dma((groups,)),
            dma((outer, groups)),
            dma((sp_count, groups)),
            dma,
            dma,
            dma((tp_count,)),
            dma((tp_count,)),
            dma((tp_count,)),
            dma((tp_count,)),
            dma((tp_count,)),
            dma((tp_count,)),
            dma((tp_count,)),
            dma((tp_count,)),
        ],
        compiler_params=pltpu.CompilerParams(
            collective_id=0, has_side_effects=True, vmem_limit_bytes=60 * 1024 * 1024
        ),
    )(*arguments)


def solution(mesh):
    in_specs = (
        P(("sp", "tp"), None),
        P(),
        P(None, "tp"),
        P(None, "tp"),
        P(None, "tp"),
        P("tp"),
        P(None, "tp"),
        P(None, "tp"),
        P(None, "tp"),
        P(None, "tp"),
        P(None, "tp"),
        P("tp"),
        P("tp"),
        P("tp"),
        P("tp", None),
        P("tp", None),
        P("tp"),
    )
    body = partial(shards, mesh.shape["sp"], mesh.shape["tp"])
    return jax.shard_map(
        body, mesh=mesh, in_specs=in_specs, out_specs=P("sp", "tp"), check_vma=False
    )
```

```python
from functools import partial
import math

import jax
import jax.numpy as jnp
from jax import lax
from jax.experimental import pallas as pl
from jax.experimental.pallas import tpu as pltpu
from jax.sharding import PartitionSpec as P

HEAD_DIM = 128
WIDTH = 31
EPSILON = 1e-06
HALO = 32
MESH = pl.DeviceIdType.MESH


def mm(left, right):
    return jnp.dot(left, right, preferred_element_type=jnp.float32)


def row(ref):
    return ref[...].reshape(1, ref.shape[0])


def whole_layer(
    sp_count,
    tp_count,
    pair,
    hidden_in,
    pre_gain,
    w_query,
    w_key,
    w_value,
    stick_offset,
    w_glu_a,
    w_glu_b,
    w_gate_attn,
    w_gate_conv,
    conv_taps,
    conv_bias,
    norm_gain,
    norm_shift,
    w_attn_out,
    w_conv_out,
    post_gain,
    out,
    hidden_all,
    pre_gain_v,
    wq,
    wk,
    wv,
    wa,
    wb,
    wga,
    wgc,
    taps,
    bias,
    gain,
    shift,
    wo,
    wc,
    post_gain_v,
    normed,
    kv,
    gated,
    gated_f32,
    attn_out,
    attn_in,
    conv_out,
    conv_in,
    stat_out,
    stat_in,
    square_out,
    square_in,
    local_sem,
    ready,
    hidden_send,
    hidden_recv,
    column_send,
    across_send,
    relay_send,
    kv_recv,
    halo_send,
    halo_recv,
    attn_send,
    attn_recv,
    conv_send,
    conv_recv,
    stat_send,
    stat_recv,
    square_send,
    square_recv,
):
    part, width = hidden_in.shape
    rows = part * tp_count
    channels = w_glu_a.shape[1]
    kv_width = w_key.shape[1]
    heads = stick_offset.shape[0]
    out_cols = post_gain.shape[0]
    outer = sp_count // pair
    size = 2 if tp_count % 2 == 0 else 1
    groups = tp_count // size
    sp = lax.axis_index("sp")
    tp = lax.axis_index("tp")
    z, x = sp // pair, sp % pair
    f32, bf16 = jnp.float32, jnp.bfloat16

    local_pairs = (
        (hidden_in, hidden_all.at[tp]),
        (pre_gain, pre_gain_v),
        (w_key, wk),
        (w_value, wv),
        (w_glu_a, wa),
        (w_glu_b, wb),
        (w_query, wq),
        (conv_taps, taps),
        (conv_bias, bias),
        (norm_gain, gain),
        (norm_shift, shift),
        (w_gate_attn, wga),
        (w_gate_conv, wgc),
        (w_conv_out, wc),
        (w_attn_out, wo),
        (post_gain, post_gain_v),
    )
    loads = [
        pltpu.make_async_copy(source, target, local_sem.at[index])
        for index, (source, target) in enumerate(local_pairs)
    ]
    (
        l_hidden, l_pre, l_key, l_value, l_a, l_b, l_query, l_taps, l_bias, l_gain, l_shift,
        l_ga, l_gc, l_wc, l_wo, l_post,
    ) = loads
    for load in loads:
        load.start()

    barrier = pltpu.get_barrier_semaphore()

    def greet(sp_index, tp_index):
        pl.semaphore_signal(barrier, inc=1, device_id=(sp_index, tp_index), device_id_type=MESH)

    for step in range(1, tp_count):
        greet(sp, lax.rem(tp + step, tp_count))
    if pair == 2:
        greet(z * pair + (1 - x), tp)

    @pl.when(z > 0)
    def _():
        greet(sp - pair, tp)

    @pl.when(z < outer - 1)
    def _():
        greet(sp + pair, tp)

    beside = jnp.where(z > 0, 1, 0) + jnp.where(z < outer - 1, 1, 0)
    pl.semaphore_wait(barrier, tp_count - 1 + (pair - 1) + beside)

    def remote(source, target, send_sem, recv_sem, sp_index, tp_index):
        return pltpu.make_async_remote_copy(
            src_ref=source,
            dst_ref=target,
            send_sem=send_sem,
            recv_sem=recv_sem,
            device_id=(sp_index, tp_index),
            device_id_type=MESH,
        )

    peers = [
        lax.rem(tp // size + group, groups) * size + lax.rem(tp + member, size)
        for group in [*range(1, groups), 0]
        for member in range(1 if group == 0 else 0, size)
    ]
    senders = peers[::-1]

    def exchange(source, target, send_sem, recv_sem, peer, varied):
        piece = source.at[peer] if varied else source
        return remote(piece, target.at[tp], send_sem.at[peer], recv_sem.at[tp], sp, peer)

    def arrival(target, send_sem, recv_sem, peer):
        return remote(
            target.at[peer], target.at[peer], send_sem.at[peer], recv_sem.at[peer], sp, peer
        )

    l_hidden.wait()
    hidden_copies = [
        exchange(hidden_all.at[tp], hidden_all, hidden_send, hidden_recv, peer, False)
        for peer in peers
    ]
    for copy in hidden_copies:
        copy.start()

    @pl.when(z < outer - 1)
    def _():
        pl.semaphore_wait(ready, 1)

    @pl.when(z > 0)
    def _():
        pl.semaphore_signal(ready, inc=1, device_id=(sp - pair, tp), device_id_type=MESH)

    l_pre.wait()

    def project(weight):
        return mm(normed[...], weight[...]).astype(bf16)

    def group_rows(group):
        first = lax.rem(tp // size + group, groups) * (size * part)
        return pl.ds(pl.multiple_of(first, size * part), size * part)

    def kv_copy(block, group, send_sem, sp_index):
        piece = kv.at[block, group_rows(group)]
        return remote(piece, piece, send_sem, kv_recv.at[block, group], sp_index, tp)

    def column_copy(target_z, group):
        return kv_copy(sp, group, column_send.at[target_z, group], target_z * pair + x)

    def across_copy(group):
        return kv_copy(sp, group, across_send.at[group], sp + 1)

    def relay_copy(source_z, group):
        return kv_copy(
            source_z * pair + x, group, relay_send.at[source_z, group], z * pair + (1 - x)
        )

    def block_arrival(block, group):
        piece = kv.at[block, group_rows(group)]
        return remote(
            piece, piece, across_send.at[group], kv_recv.at[block, group], sp,
            lax.rem(tp + 1, tp_count),
        )

    def relay(source_z, group):
        block_arrival(source_z * pair + x, group).wait_recv()
        if pair == 2:
            relay_copy(source_z, group).start()

    for group in range(groups):
        for member in range(size):
            index = lax.rem(tp // size + group, groups) * size + member
            if group == 0:

                @pl.when(index != tp)
                def _():
                    arrival(hidden_all, hidden_send, hidden_recv, index).wait_recv()

            else:
                arrival(hidden_all, hidden_send, hidden_recv, index).wait_recv()
            values = hidden_all[index].astype(f32)
            inverse = lax.rsqrt(jnp.mean(values * values, axis=1, keepdims=True) + EPSILON)
            normed[pl.ds(pl.multiple_of(index * part, part), part), :] = (
                values * inverse * row(pre_gain_v)
            ).astype(bf16)
        if group == 0:
            l_key.wait()
            l_value.wait()
        tokens = normed[group_rows(group), :]
        kv[sp, group_rows(group), :kv_width] = mm(tokens, wk[...]).astype(bf16)
        kv[sp, group_rows(group), kv_width:] = mm(tokens, wv[...]).astype(bf16)
        if pair == 2:

            @pl.when(x == 0)
            def _():
                across_copy(group).start()

        @pl.loop(z + 1, outer)
        def _(turn):
            column_copy(outer + z - turn, group).start()

    if pair == 2:

        @pl.when(x == 0)
        def _():
            kv[sp + 1] = jnp.zeros(kv.shape[1:], bf16)

    def early_relay(group, step):
        if step <= early and group < groups:

            @pl.when(z >= step)
            def _():
                relay(z - step, group)

    early = min(outer - 1, 3)

    l_a.wait()
    left = project(wa).astype(f32)
    l_b.wait()
    right = project(wb).astype(f32)
    gated[HALO:, :] = (left * jax.nn.sigmoid(right)).astype(bf16)

    def halo_copy():
        return remote(
            gated.at[pl.ds(rows, HALO)], gated.at[pl.ds(0, HALO)], halo_send, halo_recv,
            jnp.minimum(sp + 1, sp_count - 1) if pair == 1 else sp + 1, tp,
        )

    @pl.when(sp < sp_count - 1)
    def _():
        halo_copy().start()

    @pl.when(sp == 0)
    def _():
        gated[:HALO, :] = jnp.zeros((HALO, channels), bf16)

    early_relay(0, 1)
    l_query.wait()
    queries = project(wq)

    l_ga.wait()
    gate_attn = jax.nn.sigmoid(project(wga).astype(f32))
    early_relay(0, 2)

    @pl.when(sp > 0)
    def _():
        halo_copy().wait_recv()

    for load in (l_taps, l_bias, l_gain, l_shift):
        load.wait()
    gated_f32[...] = gated[...].astype(f32)
    sums = [jnp.broadcast_to(row(bias), (rows, channels))] + [jnp.zeros((rows, channels), f32)] * 3
    for tap in range(WIDTH):
        first = HALO - (WIDTH - 1) + tap
        sums[tap % 4] = sums[tap % 4] + taps[tap : tap + 1, :] * gated_f32[first : first + rows, :]
    convolved = (sums[0] + sums[1]) + (sums[2] + sums[3])

    def turned(columns):
        lane = lax.broadcasted_iota(jnp.int32, (rows, 128), 1)
        tile = jnp.zeros((rows, 128), f32)
        for index, column in enumerate(columns):
            tile = jnp.where(lane == index, column, tile)
        return jnp.transpose(tile)[:8, :]

    def turned_back(tile):
        full = jnp.concatenate([tile, jnp.zeros((120, rows), f32)], axis=0)
        return jnp.transpose(full)

    stat_out[...] = turned(
        [
            jnp.sum(convolved, axis=1, keepdims=True),
            jnp.sum(convolved * convolved, axis=1, keepdims=True),
        ]
    )
    for peer in peers:
        exchange(stat_out, stat_in, stat_send, stat_recv, peer, False).start()

    early_relay(0, 3)
    l_gc.wait()
    gate_conv = jax.nn.sigmoid(project(wgc).astype(f32))
    early_relay(1, 1)

    stacked = heads * rows
    scale = 1.0 / math.sqrt(HEAD_DIM)
    keys_step = pair * rows
    offset_column = jnp.concatenate(
        [jnp.full((rows, 1), stick_offset[head], f32) for head in range(heads)], axis=0
    )
    later = (
        lax.broadcasted_iota(jnp.int32, (keys_step, keys_step), 0)
        > lax.broadcasted_iota(jnp.int32, (keys_step, keys_step), 1)
    ).astype(bf16)

    def attend(pair_index, state, causal):
        total, summed = state
        blocks = kv[pl.ds(pair_index * pair, pair)].reshape(keys_step, 2 * kv_width)
        scores = jnp.concatenate(
            [
                lax.dot_general(
                    queries[:, head * HEAD_DIM : (head + 1) * HEAD_DIM],
                    blocks[:, head * HEAD_DIM : (head + 1) * HEAD_DIM],
                    (((1,), (1,)), ((), ())),
                    preferred_element_type=f32,
                )
                for head in range(heads)
            ],
            axis=0,
        )
        scores = scores * scale + offset_column
        small = jnp.log(1.0 + jnp.exp(-jnp.abs(scores)))
        rest = -(jnp.maximum(scores, 0.0) + small)
        if causal is not None:
            rest = jnp.where(causal, rest, 0.0)
        high = rest.astype(bf16)
        low = (rest - high.astype(f32)).astype(bf16)
        inside = mm(high, later) + mm(low, later)
        weights = jnp.exp(jnp.minimum(scores, 0.0) - small + inside + total)
        if causal is not None:
            weights = jnp.where(causal, weights, 0.0)
        weights = weights.astype(bf16)
        added = jnp.concatenate(
            [
                mm(
                    weights[head * rows : (head + 1) * rows],
                    blocks[:, kv_width + head * HEAD_DIM : kv_width + (head + 1) * HEAD_DIM],
                )
                for head in range(heads)
            ],
            axis=0,
        )
        return (total + jnp.sum(rest, axis=1, keepdims=True), summed + added)

    if pair == 2:

        @pl.when(x == 1)
        def _():
            for group in range(groups):
                block_arrival(sp - 1, group).wait_recv()

    token = lax.broadcasted_iota(jnp.int32, (rows, keys_step), 0)
    token = jnp.concatenate([token] * heads, axis=0) + x * rows
    causal = lax.broadcasted_iota(jnp.int32, (stacked, keys_step), 1) < token
    state = attend(
        z, (jnp.zeros((stacked, 1), f32), jnp.zeros((stacked, HEAD_DIM), f32)), causal
    )

    stats = stat_out[...]
    for peer in senders:
        arrival(stat_in, stat_send, stat_recv, peer).wait_recv()
        stats = stats + stat_in[peer]
    stats = turned_back(stats) / (channels * tp_count)
    mean = stats[:, 0:1]
    spread = stats[:, 1:2] - mean * mean
    conv_normed = jax.nn.silu(
        (convolved - mean) * lax.rsqrt(spread + EPSILON) * row(gain) + row(shift)
    ).astype(bf16)

    def branch(values, weight, sent, received, send_sem, recv_sem):
        def term(peer):
            return mm(values, weight[:, pl.ds(pl.multiple_of(peer * out_cols, 128), out_cols)])

        for peer in peers:
            sent[peer] = term(peer).astype(bf16)
            exchange(sent, received, send_sem, recv_sem, peer, True).start()
        return term(tp)

    def branch_sum(own, received, send_sem, recv_sem):
        for peer in senders:
            arrival(received, send_sem, recv_sem, peer).wait_recv()
            own = own + received[peer].astype(f32)
        return own.astype(bf16).astype(f32)

    l_wc.wait()
    conv_own = branch(conv_normed, wc, conv_out, conv_in, conv_send, conv_recv)

    @pl.loop(early + 1, z + 1)
    def _(step):
        relay(z - step, 0)

    def earlier(step, state):
        source_z = z - step
        for group in range(1, groups):
            if group > 1:
                relay(source_z, group)
            else:

                @pl.when(step < z)
                def _():
                    relay(source_z - 1, group)

        if pair == 2:
            for group in range(groups):
                block_arrival(source_z * pair + (1 - x), group).wait_recv()
        return attend(source_z, state, None)

    _, summed = lax.fori_loop(1, z + 1, earlier, state)
    attended = jnp.concatenate(
        [summed[head * rows : (head + 1) * rows] for head in range(heads)], axis=1
    ).astype(bf16)

    l_wo.wait()
    attn_own = branch(attended, wo, attn_out, attn_in, attn_send, attn_recv)
    merged = gate_conv * branch_sum(conv_own, conv_in, conv_send, conv_recv)
    merged = gate_attn * branch_sum(attn_own, attn_in, attn_send, attn_recv) + merged

    square_out[...] = turned([jnp.sum(merged * merged, axis=1, keepdims=True)])
    for peer in peers:
        exchange(square_out, square_in, square_send, square_recv, peer, False).start()
    l_post.wait()
    scaled = merged * row(post_gain_v)
    squares = square_out[...]
    for peer in senders:
        arrival(square_in, square_send, square_recv, peer).wait_recv()
        squares = squares + square_in[peer]
    squares = turned_back(squares)[:, 0:1]
    out[...] = (scaled * lax.rsqrt(squares / width + EPSILON)).astype(bf16)

    for peer in peers:
        exchange(hidden_all.at[tp], hidden_all, hidden_send, hidden_recv, peer, False).wait_send()
        exchange(stat_out, stat_in, stat_send, stat_recv, peer, False).wait_send()
        exchange(conv_out, conv_in, conv_send, conv_recv, peer, True).wait_send()
        exchange(attn_out, attn_in, attn_send, attn_recv, peer, True).wait_send()
        exchange(square_out, square_in, square_send, square_recv, peer, False).wait_send()
    for group in range(groups):
        if pair == 2:

            @pl.when(x == 0)
            def _():
                across_copy(group).wait_send()

            @pl.loop(0, z)
            def _(source_z):
                relay_copy(source_z, group).wait_send()

        @pl.loop(z + 1, outer)
        def _(target_z):
            column_copy(target_z, group).wait_send()

    @pl.when(sp < sp_count - 1)
    def _():
        halo_copy().wait_send()


def shards(sp_count, tp_count, *arguments):
    (
        hidden_in, pre_gain, w_query, w_key, w_value, stick_offset, w_glu_a, w_glu_b,
        w_gate_attn, w_gate_conv, conv_taps, conv_bias, norm_gain, norm_shift,
        w_attn_out, w_conv_out, post_gain,
    ) = arguments
    pair = 2 if sp_count % 2 == 0 else 1
    part, width = hidden_in.shape
    rows = part * tp_count
    channels = w_glu_a.shape[1]
    kv_width = w_key.shape[1]
    out_cols = post_gain.shape[0]
    outer = sp_count // pair
    groups = tp_count // (2 if tp_count % 2 == 0 else 1)
    f32, bf16 = jnp.float32, jnp.bfloat16
    dma = pltpu.SemaphoreType.DMA

    def like(array):
        return pltpu.VMEM(array.shape, array.dtype)

    in_specs = [
        pl.BlockSpec(memory_space=pltpu.SMEM if index == 5 else pl.ANY)
        for index in range(len(arguments))
    ]
    branch_shape = (tp_count, rows, out_cols)
    return pl.pallas_call(
        partial(whole_layer, sp_count, tp_count, pair),
        out_shape=jax.ShapeDtypeStruct((rows, out_cols), bf16),
        in_specs=in_specs,
        out_specs=pl.BlockSpec(memory_space=pltpu.VMEM),
        scratch_shapes=[
            pltpu.VMEM((tp_count, part, width), bf16),
            like(pre_gain),
            like(w_query),
            like(w_key),
            like(w_value),
            like(w_glu_a),
            like(w_glu_b),
            like(w_gate_attn),
            like(w_gate_conv),
            like(conv_taps),
            like(conv_bias),
            like(norm_gain),
            like(norm_shift),
            like(w_attn_out),
            like(w_conv_out),
            like(post_gain),
            pltpu.VMEM((rows, width), bf16),
            pltpu.VMEM((sp_count, rows, 2 * kv_width), bf16),
            pltpu.VMEM((HALO + rows, channels), bf16),
            pltpu.VMEM((HALO + rows, channels), f32),
            pltpu.VMEM(branch_shape, bf16),
            pltpu.VMEM(branch_shape, bf16),
            pltpu.VMEM(branch_shape, bf16),
            pltpu.VMEM(branch_shape, bf16),
            pltpu.VMEM((8, rows), f32),
            pltpu.VMEM((tp_count, 8, rows), f32),
            pltpu.VMEM((8, rows), f32),
            pltpu.VMEM((tp_count, 8, rows), f32),
            dma((16,)),
            pltpu.SemaphoreType.REGULAR,
            dma((tp_count,)),
            dma((tp_count,)),
            dma((outer, groups)),
            dma((groups,)),
            dma((outer, groups)),
            dma((sp_count, groups)),
            dma,
            dma,
            dma((tp_count,)),
            dma((tp_count,)),
            dma((tp_count,)),
            dma((tp_count,)),
            dma((tp_count,)),
            dma((tp_count,)),
            dma((tp_count,)),
            dma((tp_count,)),
        ],
        compiler_params=pltpu.CompilerParams(
            collective_id=0, has_side_effects=True, vmem_limit_bytes=60 * 1024 * 1024
        ),
    )(*arguments)


def solution(mesh):
    in_specs = (
        P(("sp", "tp"), None),
        P(),
        P(None, "tp"),
        P(None, "tp"),
        P(None, "tp"),
        P("tp"),
        P(None, "tp"),
        P(None, "tp"),
        P(None, "tp"),
        P(None, "tp"),
        P(None, "tp"),
        P("tp"),
        P("tp"),
        P("tp"),
        P("tp", None),
        P("tp", None),
        P("tp"),
    )
    body = partial(shards, mesh.shape["sp"], mesh.shape["tp"])
    return jax.shard_map(
        body, mesh=mesh, in_specs=in_specs, out_specs=P("sp", "tp"), check_vma=False
    )
```

```python
from functools import partial
import math

import jax
import jax.numpy as jnp
from jax import lax
from jax.experimental import pallas as pl
from jax.experimental.pallas import tpu as pltpu
from jax.sharding import PartitionSpec as P

HEAD_DIM = 128
WIDTH = 31
EPSILON = 1e-06
HALO = 32
MESH = pl.DeviceIdType.MESH


def mm(left, right):
    return jnp.dot(left, right, preferred_element_type=jnp.float32)


def row(ref):
    return ref[...].reshape(1, ref.shape[0])


def whole_layer(
    sp_count,
    tp_count,
    pair,
    hidden_in,
    pre_gain,
    w_query,
    w_key,
    w_value,
    stick_offset,
    w_glu_a,
    w_glu_b,
    w_gate_attn,
    w_gate_conv,
    conv_taps,
    conv_bias,
    norm_gain,
    norm_shift,
    w_attn_out,
    w_conv_out,
    post_gain,
    out,
    hidden_all,
    pre_gain_v,
    wq,
    wk,
    wv,
    wa,
    wb,
    wga,
    wgc,
    taps,
    bias,
    gain,
    shift,
    wo,
    wc,
    post_gain_v,
    normed,
    kv,
    gated,
    gated_f32,
    attn_out,
    attn_in,
    conv_out,
    conv_in,
    stat_out,
    stat_in,
    square_out,
    square_in,
    local_sem,
    ready,
    hidden_send,
    hidden_recv,
    column_send,
    across_send,
    relay_send,
    kv_recv,
    halo_send,
    halo_recv,
    attn_send,
    attn_recv,
    conv_send,
    conv_recv,
    stat_send,
    stat_recv,
    square_send,
    square_recv,
):
    part, width = hidden_in.shape
    rows = part * tp_count
    channels = w_glu_a.shape[1]
    kv_width = w_key.shape[1]
    heads = stick_offset.shape[0]
    out_cols = post_gain.shape[0]
    outer = sp_count // pair
    size = 2 if tp_count % 2 == 0 else 1
    groups = tp_count // size
    sp = lax.axis_index("sp")
    tp = lax.axis_index("tp")
    z, x = sp // pair, sp % pair
    f32, bf16 = jnp.float32, jnp.bfloat16

    local_pairs = (
        (hidden_in, hidden_all.at[tp]),
        (pre_gain, pre_gain_v),
        (w_key, wk),
        (w_value, wv),
        (w_glu_a, wa),
        (w_glu_b, wb),
        (w_query, wq),
        (conv_taps, taps),
        (conv_bias, bias),
        (norm_gain, gain),
        (norm_shift, shift),
        (w_gate_attn, wga),
        (w_gate_conv, wgc),
        (w_conv_out, wc),
        (w_attn_out, wo),
        (post_gain, post_gain_v),
    )
    loads = [
        pltpu.make_async_copy(source, target, local_sem.at[index])
        for index, (source, target) in enumerate(local_pairs)
    ]
    (
        l_hidden, l_pre, l_key, l_value, l_a, l_b, l_query, l_taps, l_bias, l_gain, l_shift,
        l_ga, l_gc, l_wc, l_wo, l_post,
    ) = loads
    for load in loads:
        load.start()

    barrier = pltpu.get_barrier_semaphore()

    def greet(sp_index, tp_index):
        pl.semaphore_signal(barrier, inc=1, device_id=(sp_index, tp_index), device_id_type=MESH)

    for step in range(1, tp_count):
        greet(sp, lax.rem(tp + step, tp_count))
    if pair == 2:
        greet(z * pair + (1 - x), tp)

    @pl.when(z > 0)
    def _():
        greet(sp - pair, tp)

    @pl.when(z < outer - 1)
    def _():
        greet(sp + pair, tp)

    beside = jnp.where(z > 0, 1, 0) + jnp.where(z < outer - 1, 1, 0)
    pl.semaphore_wait(barrier, tp_count - 1 + (pair - 1) + beside)

    def remote(source, target, send_sem, recv_sem, sp_index, tp_index):
        return pltpu.make_async_remote_copy(
            src_ref=source,
            dst_ref=target,
            send_sem=send_sem,
            recv_sem=recv_sem,
            device_id=(sp_index, tp_index),
            device_id_type=MESH,
        )

    peers = [
        lax.rem(tp // size + group, groups) * size + lax.rem(tp + member, size)
        for group in [*range(1, groups), 0]
        for member in range(1 if group == 0 else 0, size)
    ]
    senders = peers[::-1]

    def exchange(source, target, send_sem, recv_sem, peer, varied):
        piece = source.at[peer] if varied else source
        return remote(piece, target.at[tp], send_sem.at[peer], recv_sem.at[tp], sp, peer)

    def arrival(target, send_sem, recv_sem, peer):
        return remote(
            target.at[peer], target.at[peer], send_sem.at[peer], recv_sem.at[peer], sp, peer
        )

    l_hidden.wait()
    hidden_copies = [
        exchange(hidden_all.at[tp], hidden_all, hidden_send, hidden_recv, peer, False)
        for peer in peers
    ]
    for copy in hidden_copies:
        copy.start()

    @pl.when(z < outer - 1)
    def _():
        pl.semaphore_wait(ready, 1)

    @pl.when(z > 0)
    def _():
        pl.semaphore_signal(ready, inc=1, device_id=(sp - pair, tp), device_id_type=MESH)

    l_pre.wait()

    def project(weight):
        return mm(normed[...], weight[...]).astype(bf16)

    def group_rows(group):
        first = lax.rem(tp // size + group, groups) * (size * part)
        return pl.ds(pl.multiple_of(first, size * part), size * part)

    def kv_copy(block, group, send_sem, sp_index):
        piece = kv.at[block, group_rows(group)]
        return remote(piece, piece, send_sem, kv_recv.at[block, group], sp_index, tp)

    def column_copy(target_z, group):
        return kv_copy(sp, group, column_send.at[target_z, group], target_z * pair + x)

    def across_copy(group):
        return kv_copy(sp, group, across_send.at[group], sp + 1)

    def relay_copy(source_z, group):
        return kv_copy(
            source_z * pair + x, group, relay_send.at[source_z, group], z * pair + (1 - x)
        )

    def block_arrival(block, group):
        piece = kv.at[block, group_rows(group)]
        return remote(
            piece, piece, across_send.at[group], kv_recv.at[block, group], sp,
            lax.rem(tp + 1, tp_count),
        )

    def relay(source_z, group):
        block_arrival(source_z * pair + x, group).wait_recv()
        if pair == 2:
            relay_copy(source_z, group).start()

    for group in range(groups):
        for member in range(size):
            index = lax.rem(tp // size + group, groups) * size + member
            if group == 0:

                @pl.when(index != tp)
                def _():
                    arrival(hidden_all, hidden_send, hidden_recv, index).wait_recv()

            else:
                arrival(hidden_all, hidden_send, hidden_recv, index).wait_recv()
            values = hidden_all[index].astype(f32)
            inverse = lax.rsqrt(jnp.mean(values * values, axis=1, keepdims=True) + EPSILON)
            normed[pl.ds(pl.multiple_of(index * part, part), part), :] = (
                values * inverse * row(pre_gain_v)
            ).astype(bf16)
        if group == 0:
            l_key.wait()
            l_value.wait()
        tokens = normed[group_rows(group), :]
        kv[sp, group_rows(group), :kv_width] = mm(tokens, wk[...]).astype(bf16)
        kv[sp, group_rows(group), kv_width:] = mm(tokens, wv[...]).astype(bf16)
        if pair == 2:

            @pl.when(x == 0)
            def _():
                across_copy(group).start()

        @pl.loop(z + 1, outer)
        def _(turn):
            column_copy(outer + z - turn, group).start()

    if pair == 2:

        @pl.when(x == 0)
        def _():
            kv[sp + 1] = jnp.zeros(kv.shape[1:], bf16)

    def early_relay(group, step):
        if step <= early and group < groups:

            @pl.when(z >= step)
            def _():
                relay(z - step, group)

    early = min(outer - 1, 3)

    l_a.wait()
    left = project(wa).astype(f32)
    l_b.wait()
    right = project(wb).astype(f32)
    gated[HALO:, :] = (left * jax.nn.sigmoid(right)).astype(bf16)

    def halo_copy():
        return remote(
            gated.at[pl.ds(rows, HALO)], gated.at[pl.ds(0, HALO)], halo_send, halo_recv,
            jnp.minimum(sp + 1, sp_count - 1) if pair == 1 else sp + 1, tp,
        )

    @pl.when(sp < sp_count - 1)
    def _():
        halo_copy().start()

    @pl.when(sp == 0)
    def _():
        gated[:HALO, :] = jnp.zeros((HALO, channels), bf16)

    early_relay(0, 1)
    l_query.wait()
    queries = project(wq)

    l_ga.wait()
    gate_attn = jax.nn.sigmoid(project(wga).astype(f32))
    early_relay(0, 2)

    @pl.when(sp > 0)
    def _():
        halo_copy().wait_recv()

    for load in (l_taps, l_bias, l_gain, l_shift):
        load.wait()
    gated_f32[...] = gated[...].astype(f32)
    sums = [jnp.broadcast_to(row(bias), (rows, channels))] + [jnp.zeros((rows, channels), f32)] * 3
    for tap in range(WIDTH):
        first = HALO - (WIDTH - 1) + tap
        sums[tap % 4] = sums[tap % 4] + taps[tap : tap + 1, :] * gated_f32[first : first + rows, :]
    convolved = (sums[0] + sums[1]) + (sums[2] + sums[3])

    def turned(columns):
        lane = lax.broadcasted_iota(jnp.int32, (rows, 128), 1)
        tile = jnp.zeros((rows, 128), f32)
        for index, column in enumerate(columns):
            tile = jnp.where(lane == index, column, tile)
        return jnp.transpose(tile)[:8, :]

    def turned_back(tile):
        full = jnp.concatenate([tile, jnp.zeros((120, rows), f32)], axis=0)
        return jnp.transpose(full)

    stat_out[...] = turned(
        [
            jnp.sum(convolved, axis=1, keepdims=True),
            jnp.sum(convolved * convolved, axis=1, keepdims=True),
        ]
    )
    for peer in peers:
        exchange(stat_out, stat_in, stat_send, stat_recv, peer, False).start()

    early_relay(0, 3)
    l_gc.wait()
    gate_conv = jax.nn.sigmoid(project(wgc).astype(f32))
    early_relay(1, 1)

    stacked = heads * rows
    scale = 1.0 / math.sqrt(HEAD_DIM)
    keys_step = pair * rows
    offset_column = jnp.concatenate(
        [jnp.full((rows, 1), stick_offset[head], f32) for head in range(heads)], axis=0
    )
    later = (
        lax.broadcasted_iota(jnp.int32, (keys_step, keys_step), 0)
        > lax.broadcasted_iota(jnp.int32, (keys_step, keys_step), 1)
    ).astype(bf16)

    def attend(pair_index, state, causal):
        total, summed = state
        blocks = kv[pl.ds(pair_index * pair, pair)].reshape(keys_step, 2 * kv_width)
        scores = jnp.concatenate(
            [
                lax.dot_general(
                    queries[:, head * HEAD_DIM : (head + 1) * HEAD_DIM],
                    blocks[:, head * HEAD_DIM : (head + 1) * HEAD_DIM],
                    (((1,), (1,)), ((), ())),
                    preferred_element_type=f32,
                )
                for head in range(heads)
            ],
            axis=0,
        )
        scores = scores * scale + offset_column
        small = jnp.log(1.0 + jnp.exp(-jnp.abs(scores)))
        rest = -(jnp.maximum(scores, 0.0) + small)
        if causal is not None:
            rest = jnp.where(causal, rest, 0.0)
        high = rest.astype(bf16)
        low = (rest - high.astype(f32)).astype(bf16)
        inside = mm(high, later) + mm(low, later)
        weights = jnp.exp(jnp.minimum(scores, 0.0) - small + inside + total)
        if causal is not None:
            weights = jnp.where(causal, weights, 0.0)
        weights = weights.astype(bf16)
        added = jnp.concatenate(
            [
                mm(
                    weights[head * rows : (head + 1) * rows],
                    blocks[:, kv_width + head * HEAD_DIM : kv_width + (head + 1) * HEAD_DIM],
                )
                for head in range(heads)
            ],
            axis=0,
        )
        return (total + jnp.sum(rest, axis=1, keepdims=True), summed + added)

    if pair == 2:

        @pl.when(x == 1)
        def _():
            for group in range(groups):
                block_arrival(sp - 1, group).wait_recv()

    token = lax.broadcasted_iota(jnp.int32, (rows, keys_step), 0)
    token = jnp.concatenate([token] * heads, axis=0) + x * rows
    causal = lax.broadcasted_iota(jnp.int32, (stacked, keys_step), 1) < token
    state = attend(
        z, (jnp.zeros((stacked, 1), f32), jnp.zeros((stacked, HEAD_DIM), f32)), causal
    )

    stats = stat_out[...]
    for peer in senders:
        arrival(stat_in, stat_send, stat_recv, peer).wait_recv()
        stats = stats + stat_in[peer]
    stats = turned_back(stats) / (channels * tp_count)
    mean = stats[:, 0:1]
    spread = stats[:, 1:2] - mean * mean
    conv_normed = jax.nn.silu(
        (convolved - mean) * lax.rsqrt(spread + EPSILON) * row(gain) + row(shift)
    ).astype(bf16)

    def branch(values, weight, sent, received, send_sem, recv_sem):
        def term(peer):
            return mm(values, weight[:, pl.ds(pl.multiple_of(peer * out_cols, 128), out_cols)])

        for peer in peers:
            sent[peer] = term(peer).astype(bf16)
            exchange(sent, received, send_sem, recv_sem, peer, True).start()
        return term(tp)

    def branch_sum(own, received, send_sem, recv_sem, sources):
        for peer in sources:
            arrival(received, send_sem, recv_sem, peer).wait_recv()
            own = own + received[peer].astype(f32)
        return own.astype(bf16).astype(f32)

    l_wc.wait()
    conv_own = branch(conv_normed, wc, conv_out, conv_in, conv_send, conv_recv)

    @pl.loop(early + 1, z + 1)
    def _(step):
        relay(z - step, 0)

    def earlier(step, state):
        source_z = z - step
        for group in range(1, groups):
            if group > 1:
                relay(source_z, group)
            else:

                @pl.when(step < z)
                def _():
                    relay(source_z - 1, group)

        if pair == 2:
            for group in range(groups):
                block_arrival(source_z * pair + (1 - x), group).wait_recv()
        return attend(source_z, state, None)

    _, summed = lax.fori_loop(1, z + 1, earlier, state)
    attended = jnp.concatenate(
        [summed[head * rows : (head + 1) * rows] for head in range(heads)], axis=1
    ).astype(bf16)

    l_wo.wait()
    def attn_term(peer):
        return mm(attended, wo[:, pl.ds(pl.multiple_of(peer * out_cols, 128), out_cols)])

    if size == 2:
        sibling = tp + 1 - 2 * lax.rem(tp, 2)
        across = [lax.rem(tp // size + group, groups) * size for group in range(1, groups)]
        mine = [first + lax.rem(tp, 2) for first in across]
        theirs = [first + 1 - lax.rem(tp, 2) for first in across]
        for peer, other in zip(mine, theirs):
            attn_out[other] = attn_term(other).astype(bf16)
            remote(
                attn_out.at[other], attn_in.at[peer], attn_send.at[other], attn_recv.at[peer],
                sp, sibling,
            ).start()
        terms = [attn_term(peer) for peer in mine]
        attn_out[sibling] = attn_term(sibling).astype(bf16)
        exchange(attn_out, attn_in, attn_send, attn_recv, sibling, True).start()
        attn_own = attn_term(tp)
        for peer, other, term in zip(mine, theirs, terms):
            arrival(attn_in, attn_send, attn_recv, other).wait_recv()
            attn_out[peer] = (term + attn_in[other].astype(f32)).astype(bf16)
            exchange(attn_out, attn_in, attn_send, attn_recv, peer, True).start()
        attn_senders = [sibling, *mine]
    else:
        attn_own = branch(attended, wo, attn_out, attn_in, attn_send, attn_recv)
        attn_senders = senders
    merged = gate_conv * branch_sum(conv_own, conv_in, conv_send, conv_recv, senders)
    merged = gate_attn * branch_sum(attn_own, attn_in, attn_send, attn_recv, attn_senders) + merged

    square_out[...] = turned([jnp.sum(merged * merged, axis=1, keepdims=True)])
    for peer in peers:
        exchange(square_out, square_in, square_send, square_recv, peer, False).start()
    l_post.wait()
    scaled = merged * row(post_gain_v)
    squares = square_out[...]
    for peer in senders:
        arrival(square_in, square_send, square_recv, peer).wait_recv()
        squares = squares + square_in[peer]
    squares = turned_back(squares)[:, 0:1]
    out[...] = (scaled * lax.rsqrt(squares / width + EPSILON)).astype(bf16)

    for peer in peers:
        exchange(hidden_all.at[tp], hidden_all, hidden_send, hidden_recv, peer, False).wait_send()
        exchange(stat_out, stat_in, stat_send, stat_recv, peer, False).wait_send()
        exchange(conv_out, conv_in, conv_send, conv_recv, peer, True).wait_send()
        exchange(attn_out, attn_in, attn_send, attn_recv, peer, True).wait_send()
        exchange(square_out, square_in, square_send, square_recv, peer, False).wait_send()
    for group in range(groups):
        if pair == 2:

            @pl.when(x == 0)
            def _():
                across_copy(group).wait_send()

            @pl.loop(0, z)
            def _(source_z):
                relay_copy(source_z, group).wait_send()

        @pl.loop(z + 1, outer)
        def _(target_z):
            column_copy(target_z, group).wait_send()

    @pl.when(sp < sp_count - 1)
    def _():
        halo_copy().wait_send()


def shards(sp_count, tp_count, *arguments):
    (
        hidden_in, pre_gain, w_query, w_key, w_value, stick_offset, w_glu_a, w_glu_b,
        w_gate_attn, w_gate_conv, conv_taps, conv_bias, norm_gain, norm_shift,
        w_attn_out, w_conv_out, post_gain,
    ) = arguments
    pair = 2 if sp_count % 2 == 0 else 1
    part, width = hidden_in.shape
    rows = part * tp_count
    channels = w_glu_a.shape[1]
    kv_width = w_key.shape[1]
    out_cols = post_gain.shape[0]
    outer = sp_count // pair
    groups = tp_count // (2 if tp_count % 2 == 0 else 1)
    f32, bf16 = jnp.float32, jnp.bfloat16
    dma = pltpu.SemaphoreType.DMA

    def like(array):
        return pltpu.VMEM(array.shape, array.dtype)

    in_specs = [
        pl.BlockSpec(memory_space=pltpu.SMEM if index == 5 else pl.ANY)
        for index in range(len(arguments))
    ]
    branch_shape = (tp_count, rows, out_cols)
    return pl.pallas_call(
        partial(whole_layer, sp_count, tp_count, pair),
        out_shape=jax.ShapeDtypeStruct((rows, out_cols), bf16),
        in_specs=in_specs,
        out_specs=pl.BlockSpec(memory_space=pltpu.VMEM),
        scratch_shapes=[
            pltpu.VMEM((tp_count, part, width), bf16),
            like(pre_gain),
            like(w_query),
            like(w_key),
            like(w_value),
            like(w_glu_a),
            like(w_glu_b),
            like(w_gate_attn),
            like(w_gate_conv),
            like(conv_taps),
            like(conv_bias),
            like(norm_gain),
            like(norm_shift),
            like(w_attn_out),
            like(w_conv_out),
            like(post_gain),
            pltpu.VMEM((rows, width), bf16),
            pltpu.VMEM((sp_count, rows, 2 * kv_width), bf16),
            pltpu.VMEM((HALO + rows, channels), bf16),
            pltpu.VMEM((HALO + rows, channels), f32),
            pltpu.VMEM(branch_shape, bf16),
            pltpu.VMEM(branch_shape, bf16),
            pltpu.VMEM(branch_shape, bf16),
            pltpu.VMEM(branch_shape, bf16),
            pltpu.VMEM((8, rows), f32),
            pltpu.VMEM((tp_count, 8, rows), f32),
            pltpu.VMEM((8, rows), f32),
            pltpu.VMEM((tp_count, 8, rows), f32),
            dma((16,)),
            pltpu.SemaphoreType.REGULAR,
            dma((tp_count,)),
            dma((tp_count,)),
            dma((outer, groups)),
            dma((groups,)),
            dma((outer, groups)),
            dma((sp_count, groups)),
            dma,
            dma,
            dma((tp_count,)),
            dma((tp_count,)),
            dma((tp_count,)),
            dma((tp_count,)),
            dma((tp_count,)),
            dma((tp_count,)),
            dma((tp_count,)),
            dma((tp_count,)),
        ],
        compiler_params=pltpu.CompilerParams(
            collective_id=0, has_side_effects=True, vmem_limit_bytes=60 * 1024 * 1024
        ),
    )(*arguments)


def solution(mesh):
    in_specs = (
        P(("sp", "tp"), None),
        P(),
        P(None, "tp"),
        P(None, "tp"),
        P(None, "tp"),
        P("tp"),
        P(None, "tp"),
        P(None, "tp"),
        P(None, "tp"),
        P(None, "tp"),
        P(None, "tp"),
        P("tp"),
        P("tp"),
        P("tp"),
        P("tp", None),
        P("tp", None),
        P("tp"),
    )
    body = partial(shards, mesh.shape["sp"], mesh.shape["tp"])
    return jax.shard_map(
        body, mesh=mesh, in_specs=in_specs, out_specs=P("sp", "tp"), check_vma=False
    )
```
